32 devices in a mesh: fs: 8 (over z, x), tp: 4 (over y, core).
Axes of the slice: x: 2, y: 2, z: 4, core: 2. Of those that a mesh axis runs over, the one named last changes fastest.
Arguments:
- tokens: bfloat16 [320, 4096], P('fs'), may hold values from -6 to 6
- routes: int32 [320, 2], P('fs'), may hold values from 0 to 3, all different within a row; in each aligned block of 40 rows (0 to 39, 40 to 79, ...) at most 30 rows name the same one
- route_logits: float32 [320, 2], P('fs'), may hold values from -6 to 6
- norm_gain: float32 [4096], P('fs'), may hold values from 0.1 to 1.9
- gate_weight: float32 [4, 4096, 8192], P(None, 'fs', 'tp'), may hold values from -0.09375 to 0.09375
- up_weight: float32 [4, 4096, 8192], P(None, 'fs', 'tp'), may hold values from -0.09375 to 0.09375
- down_weight: float32 [4, 4096, 8192], P(None, 'fs', 'tp'), may hold values from -0.0625 to 0.0625
Outputs:
- mixed: bfloat16 [320, 4096], P('fs', 'tp')
- gate_sampler: bfloat16 [4, 4096, 8192], P('tp', None, 'fs')
- up_sampler: bfloat16 [4, 4096, 8192], P('tp', None, 'fs')
- down_sampler: bfloat16 [4, 4096, 8192], P('tp', None, 'fs')
The draws below stay inside these ranges and needn't reach their ends.
Inputs may be any that keep to these rules, and one draw needn't show every extreme that they name: `routes`: the 2 experts of a token differ. Within the tokens of one index of fs (aligned blocks of 40 rows) no expert is named by more than 30 tokens.
All inputs are finite; a program needn't handle non-finite values.
Results may differ from the reference program's by a relative error of at most 0.01.
Values may be sent and summed in bfloat16 or wider, within the bound.
A program may use at most 192 MiB of HBM per device.

```python
import math
import jax
import jax.numpy as jnp
import numpy as np
from jax import lax

D = 4096
FF = 8192
EXPERTS = 4
TOPK = 2
TOK_DEV = 40
CAP = 30
TOKENS = 320
N_TP = 4


def block_scale(own_key, extent, pieces, least, high):
    gain = 1.0
    for dim, parts in pieces:
        heights = jax.random.uniform(jax.random.fold_in(jax.random.fold_in(own_key, 6), dim), (parts,), jnp.float32, least / len(pieces), high / len(pieces))
        gain = gain * jnp.repeat(jnp.exp(heights), extent[dim] // parts).reshape((-1,) + (1,) * (len(extent) - 1 - dim))
    return gain


def assign_block(own_key, own, number, rows, number_of, top, limit, lean):
    order = jax.random.permutation(own_key, number_of)
    heavy_load, usual = portions_of(number_of, rows * top, limit, lean, True), portions_of(number_of, rows * top, limit, lean, False)
    places = jnp.arange(number_of)

    def named(sizes, offset_by):
        used = int((sizes > 0).sum())
        fixed = max(1, used // 4)
        moved = fixed + (places - fixed + offset_by * (used - fixed)) % max(1, number_of - fixed)
        return jnp.zeros((number_of,), jnp.int32).at[order[jnp.where(places < fixed, places, moved)]].set(jnp.asarray(sizes, jnp.int32))

    sizes = jnp.where(number % 4 == 0, named(heavy_load, number // 4), named(usual, number - number // 4 - 1))
    mixed = jax.random.permutation(jax.random.fold_in(own, 3), number_of)
    donor, sink = mixed[0:number_of // 2 * 2:2], mixed[1:number_of // 2 * 2:2]
    room = jnp.minimum(sizes[donor] - 1, limit - sizes[sink]) // 2
    room = jnp.where((donor == order[0]) | (sink == order[0]) | (sizes[sink] == 0), 0, jnp.maximum(room, 0))
    moved = jax.random.randint(jax.random.fold_in(own, 4), (number_of // 2,), 0, 1 << 20) % (room + 1)
    sizes = sizes.at[donor].add(-moved).at[sink].add(moved)
    labels = jnp.searchsorted(jnp.cumsum(sizes), jnp.arange(rows * top), side="right").astype(jnp.int32)
    grid = labels.reshape(top, rows).T
    grid = grid[jax.random.permutation(jax.random.fold_in(own, 1), rows)]
    offset_by = jax.random.randint(jax.random.fold_in(own, 2), (rows, 1), 0, top)
    return jnp.take_along_axis(grid, (jnp.arange(top)[None, :] + offset_by) % top, axis=1)


def portions_of(count, total, most, slope, full):
    loads = [(1 << 20) // math.isqrt(rank ** slope) + 1 for rank in range(1, count + 1)]
    largest = most if full else min(most, max(-(-total // count), total * loads[0] // sum(loads)))
    least = 1 if total - largest >= count - 1 else 0
    holding, spare = [largest] + [least] * (count - 1), total - largest - least * (count - 1)
    while spare > 0:
        free = [i for i in range(1, count) if holding[i] < largest] or [i for i in range(1, count) if holding[i] < most]
        mass, remaining = sum([loads[i] for i in free]), spare
        for i in free:
            extra = min(most - holding[i], max(1, remaining * loads[i] // mass), spare)
            holding[i] = holding[i] + extra
            spare = spare - extra
    return np.array(holding)


def centred(key, extent, scale, reach, cuts=(), held_as=jnp.bfloat16):
    drawn = jax.random.normal(key, extent, jnp.float32) * scale
    if len(cuts) > 0:
        drawn = block_scale(key, extent, cuts, -0.22, 0.18) * drawn
    return jnp.clip(drawn, min=-reach, max=reach).astype(held_as)


def setup_inputs(seed: int = 0) -> dict:
    arg_keys = jax.random.split(jax.random.key(seed), 8)
    tokens = centred(arg_keys[0], (TOKENS, D), 1.0, 6.0, ((0, 8),))
    routes_keys = jax.random.split(jax.random.fold_in(arg_keys[1], 1), TOKENS // TOK_DEV)
    routes_turns = jax.random.permutation(jax.random.fold_in(arg_keys[1], 3), TOKENS // TOK_DEV)
    routes = jax.vmap(lambda own, number: assign_block(jax.random.fold_in(arg_keys[1], 2), own, number, TOK_DEV, EXPERTS, TOPK, CAP, 2))(routes_keys, routes_turns).reshape((TOKENS, TOPK))
    route_logits = centred(arg_keys[2], (TOKENS, TOPK), 1.5, 6.0, ((0, 8),), jnp.float32)
    norm_gain = jnp.clip(1.0 + 0.18 * jax.random.normal(arg_keys[3], (D,), jnp.float32), 0.1, 1.9)
    gate_weight = centred(arg_keys[4], (EXPERTS, D, FF), D ** -0.5, 0.09375, ((1, 8), (2, 4)), jnp.float32)
    up_weight = centred(arg_keys[5], (EXPERTS, D, FF), D ** -0.5, 0.09375, ((1, 8), (2, 4)), jnp.float32)
    down_weight = centred(arg_keys[6], (EXPERTS, D, FF), FF ** -0.5, 0.0625, ((1, 8), (2, 4)), jnp.float32)
    return {"tokens": tokens, "routes": routes, "route_logits": route_logits, "norm_gain": norm_gain, "gate_weight": gate_weight, "up_weight": up_weight, "down_weight": down_weight}


def arrange(matrix):
    experts, width, hidden_units = matrix.shape
    block = hidden_units // N_TP
    split = matrix.reshape(experts, width, N_TP, block)
    return jnp.transpose(split, (2, 1, 0, 3)).reshape(N_TP, width, experts * block)

def reference(tokens, routes, route_logits, norm_gain, gate_weight, up_weight, down_weight):
    gain_cols = norm_gain.astype(jnp.float32)[None, :, None]
    folded_gate = (gate_weight * gain_cols).astype(jnp.bfloat16)
    folded_up = (up_weight * gain_cols).astype(jnp.bfloat16)
    rounded_down = down_weight.astype(jnp.bfloat16)
    tok_float = tokens.astype(jnp.float32)
    normed = (tok_float * lax.rsqrt(lax.optimization_barrier(jnp.mean(tok_float * tok_float, axis=1, keepdims=True)) + 1e-05)).astype(jnp.bfloat16)
    shares = jax.nn.sigmoid(route_logits - route_logits[:, ::-1])
    mixed = jnp.zeros((tokens.shape[0], tokens.shape[1]), jnp.float32)
    for expert in range(EXPERTS):
        gate_act = jnp.dot(normed, folded_gate[expert], preferred_element_type=jnp.float32)
        up_act = jnp.dot(normed, folded_up[expert], preferred_element_type=jnp.float32)
        hidden = (jax.nn.silu(gate_act) * up_act).astype(jnp.bfloat16)
        expert_out = lax.dot_general(hidden, rounded_down[expert], (((1,), (1,)), ((), ())), preferred_element_type=jnp.float32)
        weight = lax.optimization_barrier(jnp.sum(jnp.where(routes == expert, shares, 0.0), axis=1))
        mixed = mixed + weight[:, None] * expert_out
    return (mixed.astype(jnp.bfloat16), arrange(folded_gate), arrange(folded_up), arrange(rounded_down))
```

```python
import functools

import jax
import jax.numpy as jnp
from jax import lax
from jax.experimental import pallas as pl
from jax.experimental.pallas import tpu as pltpu
from jax.sharding import PartitionSpec as P

VMEM_LIMIT = 40 * 1024 * 1024


def fold_kernel(w_ref, gain_ref, out_ref):
    out_ref[...] = (w_ref[...] * gain_ref[...][None]).astype(jnp.bfloat16)


def cast_kernel(w_ref, out_ref):
    out_ref[...] = w_ref[...].astype(jnp.bfloat16)


def arrange(weight, gain, spread, piece, pieces):
    experts, width, columns = weight.shape
    block, rows = columns // spread, width // pieces
    in_specs = [pl.BlockSpec((1, rows, block), lambda e, s: (e, piece, s))]
    operands = [weight]
    if gain is not None:
        in_specs.append(pl.BlockSpec((rows, 1), lambda e, s: (piece, 0)))
        operands.append(gain)
    return pl.pallas_call(
        cast_kernel if gain is None else fold_kernel,
        grid=(experts, spread),
        in_specs=in_specs,
        out_specs=pl.BlockSpec((1, rows, block), lambda e, s: (e * spread + s, 0, 0)),
        out_shape=jax.ShapeDtypeStruct((experts * spread, rows, block), jnp.bfloat16),
        compiler_params=pltpu.CompilerParams(vmem_limit_bytes=VMEM_LIMIT),
        cost_estimate=pl.CostEstimate(
            flops=experts * rows * columns,
            bytes_accessed=experts * rows * columns * 6,
            transcendentals=0,
        ),
    )(*operands)


def gate_kernel(x_ref, w_ref, act_ref, copy_ref):
    copy_ref[...] = w_ref[...]
    part = jnp.dot(x_ref[...], w_ref[0], preferred_element_type=jnp.float32)

    @pl.when(pl.program_id(0) == 0)
    def _():
        act_ref[...] = part

    @pl.when(pl.program_id(0) > 0)
    def _():
        act_ref[...] += part


def up_kernel(x_ref, w_ref, gate_ref, hidden_ref, copy_ref, acc_ref):
    copy_ref[...] = w_ref[...]
    part = jnp.dot(x_ref[...], w_ref[0], preferred_element_type=jnp.float32)

    @pl.when(pl.program_id(0) == 0)
    def _():
        acc_ref[...] = part

    @pl.when(pl.program_id(0) > 0)
    def _():
        acc_ref[...] += part

    @pl.when(pl.program_id(0) == pl.num_programs(0) - 1)
    def _():
        gate = gate_ref[...]
        hidden_ref[...] = (gate / (1.0 + jnp.exp(-gate)) * acc_ref[...]).astype(jnp.bfloat16)


def project(rows, local, gate_act=None):
    count, width, block = local.shape
    tokens = rows.shape[0]
    in_specs = [
        pl.BlockSpec((tokens, width), lambda g: (0, g)),
        pl.BlockSpec((1, width, block), lambda g: (g, 0, 0)),
    ]
    operands = [rows, local]
    scratch = []
    kernel, act_type = gate_kernel, jnp.float32
    if gate_act is not None:
        in_specs.append(pl.BlockSpec((tokens, block), lambda g: (0, 0)))
        operands.append(gate_act)
        scratch = [pltpu.VMEM((tokens, block), jnp.float32)]
        kernel, act_type = up_kernel, jnp.bfloat16
    return pl.pallas_call(
        kernel,
        grid=(count,),
        in_specs=in_specs,
        out_specs=[
            pl.BlockSpec((tokens, block), lambda g: (0, 0)),
            pl.BlockSpec((1, width, block), lambda g: (0, g, 0)),
        ],
        out_shape=[
            jax.ShapeDtypeStruct((tokens, block), act_type),
            jax.ShapeDtypeStruct((1, count * width, block), jnp.bfloat16),
        ],
        scratch_shapes=scratch,
        compiler_params=pltpu.CompilerParams(vmem_limit_bytes=VMEM_LIMIT),
        cost_estimate=pl.CostEstimate(
            flops=2 * tokens * count * width * block,
            bytes_accessed=count * width * block * 4,
            transcendentals=0,
        ),
    )(*operands)


def down_kernel(hidden_ref, weight_ref, w_ref, *rest):
    part_ref, copy_ref = rest[-2:]
    copy_ref[...] = w_ref[...]
    part = lax.dot_general(
        hidden_ref[...], w_ref[0], (((1,), (1,)), ((), ())), preferred_element_type=jnp.float32
    )
    part = part * weight_ref[...]
    part_ref[...] = part.reshape(part_ref.shape).astype(part_ref.dtype)


def project_back(hidden, weight, local, so_far, piece, pieces, fs_count, tp_count, part_type):
    count, width, block = local.shape
    tokens = hidden.shape[0]
    per_tp = count // tp_count
    in_specs = [
        pl.BlockSpec((tokens, block), lambda g: (0, 0)),
        pl.BlockSpec((tokens, 1), lambda g: (0, 0)),
        pl.BlockSpec((1, width, block), lambda g: (g, 0, 0)),
    ]
    operands = [hidden, weight, local]
    aliases = {}
    if so_far is not None:
        in_specs.append(pl.BlockSpec(memory_space=pl.ANY))
        operands.append(so_far)
        aliases = {3: 1}
    return pl.pallas_call(
        down_kernel,
        grid=(count,),
        in_specs=in_specs,
        out_specs=[
            pl.BlockSpec(
                (fs_count, 1, tokens // fs_count, width),
                lambda g: (0, g // per_tp, 0, g % per_tp),
            ),
            pl.BlockSpec((1, width, block), lambda g: (0, g * pieces + piece, 0)),
        ],
        out_shape=[
            jax.ShapeDtypeStruct(
                (fs_count, tp_count, tokens // fs_count, per_tp * width), part_type
            ),
            jax.ShapeDtypeStruct((1, count * width * pieces, block), jnp.bfloat16),
        ],
        input_output_aliases=aliases,
        compiler_params=pltpu.CompilerParams(vmem_limit_bytes=VMEM_LIMIT),
        cost_estimate=pl.CostEstimate(
            flops=2 * tokens * count * width * block,
            bytes_accessed=count * width * block * 4 + tokens * count * width * 4,
            transcendentals=0,
        ),
    )(*operands)


def swap(pieces):
    return lax.all_to_all(pieces, "fs", split_axis=0, concat_axis=0, tiled=True)


def per_device(tokens, routes, route_logits, norm_gain, gate_weight, up_weight, down_weight):
    experts, width, _ = gate_weight.shape
    fs_count, tp_count = lax.axis_size("fs"), lax.axis_size("tp")
    spread = fs_count // experts
    own, model = tokens.shape
    part_width = model // tp_count
    pieces = 2 if width % 256 == 0 else 1
    gain = norm_gain[:, None]

    gate_local = swap(arrange(gate_weight, gain, spread, 0, 1))
    up_pieces = arrange(up_weight, gain, spread, 0, 1)
    down_pieces = [arrange(down_weight, None, spread, p, pieces) for p in range(pieces)]

    tok_float = tokens.astype(jnp.float32)
    scale = lax.rsqrt(jnp.mean(tok_float * tok_float, axis=1, keepdims=True) + 1e-05)
    start = lax.axis_index("tp") * part_width
    own_cols = lax.dynamic_slice_in_dim(tokens, start, part_width, 1).astype(jnp.float32)
    normed = (own_cols * scale).astype(jnp.bfloat16)
    gathered = lax.all_gather(normed, ("fs", "tp"), axis=0, tiled=False)
    rows = (
        gathered.reshape(fs_count, tp_count, own, part_width)
        .transpose(0, 2, 1, 3)
        .reshape(fs_count * own, model)
    )
    shares = jax.nn.sigmoid(route_logits - route_logits[:, ::-1])
    expert_ids = lax.broadcasted_iota(jnp.int32, (1, 1, experts), 2)
    weights = jnp.sum(jnp.where(routes[:, :, None] == expert_ids, shares[:, :, None], 0.0), axis=1)
    all_weights = lax.all_gather(weights, "fs", axis=0, tiled=True)
    mine = lax.axis_index("fs") // spread
    weight = lax.dynamic_slice_in_dim(all_weights, mine, 1, 1)

    up_local = swap(up_pieces)
    gate_act, gate_out = project(rows, gate_local)
    hidden, up_out = project(rows, up_local, gate_act)
    down_out, sums = None, []
    for p in range(pieces):
        part, down_out = project_back(
            hidden, weight, swap(down_pieces[p]), down_out, p, pieces, fs_count, tp_count, jnp.float32
        )
        part = part.reshape((fs_count * tp_count,) + part.shape[2:])
        summed = lax.psum_scatter(part, ("fs", "tp"), scatter_dimension=0, tiled=True)
        sums.append(summed.reshape(own, part_width // width, 1, width // pieces))
    mixed = jnp.concatenate(sums, axis=2).reshape(own, part_width).astype(jnp.bfloat16)
    return (mixed, gate_out, up_out, down_out)


def solution(mesh):
    in_specs = (
        P("fs", None),
        P("fs", None),
        P("fs", None),
        P("fs"),
        P(None, "fs", "tp"),
        P(None, "fs", "tp"),
        P(None, "fs", "tp"),
    )
    out_specs = (P("fs", "tp"), P("tp", None, "fs"), P("tp", None, "fs"), P("tp", None, "fs"))
    return jax.shard_map(
        per_device, mesh=mesh, in_specs=in_specs, out_specs=out_specs, check_vma=False
    )
```

```python
import functools

import jax
import jax.numpy as jnp
from jax import lax
from jax.experimental import pallas as pl
from jax.experimental.pallas import tpu as pltpu
from jax.sharding import PartitionSpec as P

VMEM_LIMIT = 40 * 1024 * 1024


MESH = pl.DeviceIdType.MESH


def exchange_kernel(
    fs_count, tp_count, experts, pieces,
    tok_ref, routes_ref, logits_ref, gain_ref, gate_hbm, up_hbm, down_hbm,
    rows_out, weights_out, gate_out, up_out, down_out, rest_out,
    xcol, wown, stage, gate_send, up_send, down_send, rest_send,
    load_sem, send_sem, recv_sem, keep_sem, x_send, x_recv, w_send, w_recv, t_send, t_recv,
    own_sem, rest_sem,
):
    me, my_tp = lax.axis_index("fs"), lax.axis_index("tp")
    spread = fs_count // experts
    own = tok_ref.shape[0]
    width, block = stage.shape[1], stage.shape[2]
    part = xcol.shape[2]
    rows = width // pieces
    barrier = pltpu.get_barrier_semaphore()
    for s in range(1, fs_count):
        pl.semaphore_signal(
            barrier, inc=1, device_id={"fs": lax.rem(me + s, fs_count)}, device_id_type=MESH
        )
    for s in range(1, tp_count):
        pl.semaphore_signal(
            barrier, inc=1, device_id={"tp": lax.rem(my_tp + s, tp_count)}, device_id_type=MESH
        )

    def target(step):
        return lax.rem(me + fs_count // 2 + step, fs_count)

    def load(hbm, step, slot):
        dst = target(step)
        column = pl.multiple_of(lax.rem(dst, spread) * block, block)
        return pltpu.make_async_copy(
            hbm.at[dst // spread, :, pl.ds(column, block)], stage.at[slot], load_sem.at[slot]
        )

    load(gate_hbm, 0, 0).start()

    tok = tok_ref[...].astype(jnp.float32)
    scale = lax.rsqrt(jnp.mean(tok * tok, axis=1, keepdims=True) + 1e-05)
    cols = tok_ref[:, pl.ds(pl.multiple_of(my_tp * part, part), part)].astype(jnp.float32)
    xcol[me] = (cols * scale).astype(jnp.bfloat16)
    first, second = logits_ref[:, 0:1], logits_ref[:, 1:2]
    lanes = lax.broadcasted_iota(jnp.int32, (own, 128), 1)
    wown[...] = jnp.where(
        routes_ref[:, 0:1] == lanes, 1.0 / (1.0 + jnp.exp(second - first)), 0.0
    ) + jnp.where(routes_ref[:, 1:2] == lanes, 1.0 / (1.0 + jnp.exp(first - second)), 0.0)
    pl.semaphore_wait(barrier, fs_count + tp_count - 2)

    def x_copy(dst, sem):
        return pltpu.make_async_remote_copy(
            src_ref=xcol.at[me], dst_ref=xcol.at[me], send_sem=x_send.at[dst],
            recv_sem=x_recv.at[sem], device_id={"fs": dst}, device_id_type=MESH,
        )

    def w_copy(dst, sem):
        return pltpu.make_async_remote_copy(
            src_ref=wown, dst_ref=weights_out.at[me], send_sem=w_send.at[dst],
            recv_sem=w_recv.at[sem], device_id={"fs": dst}, device_id_type=MESH,
        )

    w_keep = pltpu.make_async_copy(wown, weights_out.at[me], own_sem.at[0])
    w_keep.start()
    for s in range(1, fs_count):
        dst = lax.rem(me + s, fs_count)
        x_copy(dst, me).start()
        w_copy(dst, me).start()

    weights_in = (
        (gate_hbm, gate_send, gate_out, True),
        (up_hbm, up_send, up_out, True),
        (down_hbm, down_send, down_out, False),
    )

    def w_send_copy(m, dst):
        _, held, out, _ = weights_in[m]
        return pltpu.make_async_remote_copy(
            src_ref=held.at[dst], dst_ref=out.at[me], send_sem=send_sem.at[m, dst],
            recv_sem=recv_sem.at[m, me], device_id={"fs": dst}, device_id_type=MESH,
        )

    def keep_copy(m):
        _, held, out, _ = weights_in[m]
        return pltpu.make_async_copy(held.at[me], out.at[me], keep_sem.at[m])

    t_copies = []
    for m in range(3):
        hbm, held, out, folded = weights_in[m]

        def body(step, carry, m=m, hbm=hbm, held=held, folded=folded):
            slot = lax.rem(m * fs_count + step, 2)
            dst = target(step)

            @pl.when(step + 1 < fs_count)
            def _():
                load(hbm, step + 1, 1 - slot).start()

            if m < 2:

                @pl.when(step + 1 == fs_count)
                def _():
                    load(weights_in[m + 1][0], 0, 1 - slot).start()

            load(hbm, step, slot).wait()
            if folded:
                held[dst] = (stage[slot] * gain_ref[...]).astype(jnp.bfloat16)
            else:
                held[dst] = stage[slot, :rows].astype(jnp.bfloat16)
                if pieces > 1:
                    rest_send[dst] = stage[slot, rows:].astype(jnp.bfloat16)

            @pl.when(dst == me)
            def _():
                keep_copy(m).start()

            @pl.when(dst != me)
            def _():
                w_send_copy(m, dst).start()

            return carry

        lax.fori_loop(0, fs_count, body, 0)
        if m == 0:
            for s in range(1, fs_count):
                src = lax.rem(me + s, fs_count)
                pltpu.make_async_copy(xcol.at[src], xcol.at[src], x_recv.at[src]).wait()
            for s in range(1, tp_count):
                copy = pltpu.make_async_remote_copy(
                    src_ref=xcol, dst_ref=rows_out.at[my_tp], send_sem=t_send.at[s],
                    recv_sem=t_recv.at[s], device_id={"tp": lax.rem(my_tp + s, tp_count)},
                    device_id_type=MESH,
                )
                copy.start()
                t_copies.append(copy)
            x_keep = pltpu.make_async_copy(xcol, rows_out.at[my_tp], own_sem.at[1])
            x_keep.start()
    if pieces > 1:
        rest_copy = pltpu.make_async_copy(rest_send, rest_out, rest_sem)
        rest_copy.start()
        rest_copy.wait()
    w_keep.wait()
    x_keep.wait()
    for s in range(1, tp_count):
        src = lax.rem(my_tp + tp_count - s, tp_count)
        t_copies[s - 1].wait_send()
        pltpu.make_async_copy(xcol, rows_out.at[src], t_recv.at[s]).wait()
    for s in range(1, fs_count):
        other = lax.rem(me + s, fs_count)
        x_copy(other, me).wait_send()
        w_copy(other, me).wait_send()
        pltpu.make_async_copy(wown, weights_out.at[other], w_recv.at[other]).wait()
    for m in range(3):
        _, held, out, _ = weights_in[m]
        keep_copy(m).wait()

        def finish(s, carry, m=m, held=held, out=out):
            other = lax.rem(me + s, fs_count)
            w_send_copy(m, other).wait_send()
            pltpu.make_async_copy(held.at[other], out.at[other], recv_sem.at[m, other]).wait()
            return carry

        lax.fori_loop(1, fs_count, finish, 0)


def exchange(tokens, routes, logits, gain, gate, up, down, fs_count, tp_count, pieces):
    experts, width, columns = gate.shape
    block = columns // (fs_count // experts)
    rows = width // pieces
    own, model = tokens.shape
    part = model // tp_count
    bf16, dma = jnp.bfloat16, pltpu.SemaphoreType.DMA
    vmem = pl.BlockSpec(memory_space=pltpu.VMEM)
    anywhere = pl.BlockSpec(memory_space=pl.ANY)
    return pl.pallas_call(
        functools.partial(exchange_kernel, fs_count, tp_count, experts, pieces),
        in_specs=[vmem] * 4 + [anywhere] * 3,
        out_specs=[anywhere] * 6,
        out_shape=[
            jax.ShapeDtypeStruct((tp_count, fs_count, own, part), bf16),
            jax.ShapeDtypeStruct((fs_count, own, 128), jnp.float32),
            jax.ShapeDtypeStruct((fs_count, width, block), bf16),
            jax.ShapeDtypeStruct((fs_count, width, block), bf16),
            jax.ShapeDtypeStruct((fs_count, rows, block), bf16),
            jax.ShapeDtypeStruct((fs_count, rows, block), bf16),
        ],
        scratch_shapes=[
            pltpu.VMEM((fs_count, own, part), bf16),
            pltpu.VMEM((own, 128), jnp.float32),
            pltpu.VMEM((2, width, block), jnp.float32),
            pltpu.VMEM((fs_count, width, block), bf16),
            pltpu.VMEM((fs_count, width, block), bf16),
            pltpu.VMEM((fs_count, rows, block), bf16),
            pltpu.VMEM((fs_count, rows, block), bf16),
            dma((2,)), dma((3, fs_count)), dma((3, fs_count)), dma((3,)),
            dma((fs_count,)), dma((fs_count,)), dma((fs_count,)), dma((fs_count,)),
            dma((tp_count,)), dma((tp_count,)), dma((2,)), dma,
        ],
        compiler_params=pltpu.CompilerParams(
            collective_id=0, has_side_effects=True, vmem_limit_bytes=56 * 1024 * 1024
        ),
    )(tokens, routes, logits, gain, gate, up, down)


def reduce_kernel(
    fs_count, tp_count, experts, part_ref, out_ref, first, total, second,
    send1, recv1, send2, recv2, keep_sem,
):
    me, my_tp = lax.axis_index("fs"), lax.axis_index("tp")
    spread = fs_count // experts
    mine, half = me // spread, lax.rem(me, spread)
    group = spread * tp_count
    index = half * tp_count + my_tp
    barrier = pltpu.get_barrier_semaphore()

    def mate(s):
        other = lax.rem(index + s, group)
        return other, other // tp_count, lax.rem(other, tp_count)

    def partner(s):
        return lax.rem(mine + s, experts)

    for s in range(1, group):
        _, h, t = mate(s)
        pl.semaphore_signal(
            barrier, inc=1, device_id={"fs": mine * spread + h, "tp": t}, device_id_type=MESH
        )
    for s in range(1, experts):
        pl.semaphore_signal(
            barrier, inc=1, device_id={"fs": partner(s) * spread + half}, device_id_type=MESH
        )
    pl.semaphore_wait(barrier, group + experts - 2)

    def copy1(s):
        _, h, t = mate(s)
        return pltpu.make_async_remote_copy(
            src_ref=part_ref.at[h, t], dst_ref=first.at[s], send_sem=send1.at[s],
            recv_sem=recv1.at[s], device_id={"fs": mine * spread + h, "tp": t},
            device_id_type=MESH,
        )

    for s in range(1, group):
        copy1(s).start()
    keep = pltpu.make_async_copy(part_ref.at[half, my_tp], first.at[0], keep_sem)
    keep.start()
    keep.wait()
    acc = first[0].astype(jnp.float32)
    for s in range(1, group):
        copy1(s).wait_recv()
        acc = acc + first[s].astype(jnp.float32)
    total[...] = acc.astype(jnp.bfloat16)

    def copy2(s):
        return pltpu.make_async_remote_copy(
            src_ref=total.at[partner(s)], dst_ref=second.at[s], send_sem=send2.at[s],
            recv_sem=recv2.at[s], device_id={"fs": partner(s) * spread + half},
            device_id_type=MESH,
        )

    for s in range(1, experts):
        copy2(s).start()
    result = total[mine].astype(jnp.float32)
    for s in range(1, experts):
        copy2(s).wait_recv()
        result = result + second[s].astype(jnp.float32)
    out_ref[...] = result.astype(jnp.bfloat16)
    for s in range(1, group):
        copy1(s).wait_send()
    for s in range(1, experts):
        copy2(s).wait_send()


def reduce(part, fs_count, tp_count):
    spread, _, experts, own, columns = part.shape
    group = spread * tp_count
    bf16, dma = jnp.bfloat16, pltpu.SemaphoreType.DMA
    return pl.pallas_call(
        functools.partial(reduce_kernel, fs_count, tp_count, experts),
        in_specs=[pl.BlockSpec(memory_space=pltpu.VMEM)],
        out_specs=pl.BlockSpec(memory_space=pltpu.VMEM),
        out_shape=jax.ShapeDtypeStruct((own, columns), bf16),
        scratch_shapes=[
            pltpu.VMEM((group, experts, own, columns), bf16),
            pltpu.VMEM((experts, own, columns), bf16),
            pltpu.VMEM((experts, own, columns), bf16),
            dma((group,)), dma((group,)), dma((experts,)), dma((experts,)), dma,
        ],
        compiler_params=pltpu.CompilerParams(
            collective_id=1, has_side_effects=True, vmem_limit_bytes=48 * 1024 * 1024
        ),
    )(part)


def gate_kernel(x_ref, w_ref, act_ref, copy_ref):
    copy_ref[...] = w_ref[...]
    part = jnp.dot(x_ref[0], w_ref[0], preferred_element_type=jnp.float32)

    @pl.when(pl.program_id(0) == 0)
    def _():
        act_ref[...] = part

    @pl.when(pl.program_id(0) > 0)
    def _():
        act_ref[...] += part


def up_kernel(x_ref, w_ref, gate_ref, hidden_ref, copy_ref, acc_ref):
    copy_ref[...] = w_ref[...]
    part = jnp.dot(x_ref[0], w_ref[0], preferred_element_type=jnp.float32)

    @pl.when(pl.program_id(0) == 0)
    def _():
        acc_ref[...] = part

    @pl.when(pl.program_id(0) > 0)
    def _():
        acc_ref[...] += part

    @pl.when(pl.program_id(0) == pl.num_programs(0) - 1)
    def _():
        gate = gate_ref[...]
        hidden_ref[...] = (gate / (1.0 + jnp.exp(-gate)) * acc_ref[...]).astype(jnp.bfloat16)


def project(rows, local, gate_act=None):
    count, width, block = local.shape
    tokens = rows.shape[1]
    per_tp = count // rows.shape[0]
    in_specs = [
        pl.BlockSpec((1, tokens, width), lambda g: (g // per_tp, 0, g % per_tp)),
        pl.BlockSpec((1, width, block), lambda g: (g, 0, 0)),
    ]
    operands = [rows, local]
    scratch = []
    kernel, act_type = gate_kernel, jnp.float32
    if gate_act is not None:
        in_specs.append(pl.BlockSpec((tokens, block), lambda g: (0, 0)))
        operands.append(gate_act)
        scratch = [pltpu.VMEM((tokens, block), jnp.float32)]
        kernel, act_type = up_kernel, jnp.bfloat16
    return pl.pallas_call(
        kernel,
        grid=(count,),
        in_specs=in_specs,
        out_specs=[
            pl.BlockSpec((tokens, block), lambda g: (0, 0)),
            pl.BlockSpec((1, width, block), lambda g: (0, g, 0)),
        ],
        out_shape=[
            jax.ShapeDtypeStruct((tokens, block), act_type),
            jax.ShapeDtypeStruct((1, count * width, block), jnp.bfloat16),
        ],
        scratch_shapes=scratch,
        compiler_params=pltpu.CompilerParams(vmem_limit_bytes=VMEM_LIMIT),
        cost_estimate=pl.CostEstimate(
            flops=2 * tokens * count * width * block,
            bytes_accessed=count * width * block * 4,
            transcendentals=0,
        ),
    )(*operands)


def down_kernel(hidden_ref, weight_ref, w_ref, *rest):
    part_ref, copy_ref = rest[-2:]
    copy_ref[...] = w_ref[...]
    part = lax.dot_general(
        hidden_ref[...], w_ref[0], (((1,), (1,)), ((), ())), preferred_element_type=jnp.float32
    )
    part = part * weight_ref[...]
    spread, _, experts, own, width = part_ref.shape
    blocks = part.reshape(experts, spread, own, width).astype(part_ref.dtype)
    for h in range(spread):
        part_ref[h, 0] = blocks[:, h]


def project_back(hidden, weight, local, so_far, piece, pieces, experts, spread, tp_count):
    count, width, block = local.shape
    tokens = hidden.shape[0]
    per_tp = count // tp_count
    own = tokens // count
    in_specs = [
        pl.BlockSpec((tokens, block), lambda g: (0, 0)),
        pl.BlockSpec((tokens, 1), lambda g: (0, 0)),
        pl.BlockSpec((1, width, block), lambda g: (g, 0, 0)),
    ]
    operands = [hidden, weight, local]
    aliases = {}
    if so_far is not None:
        in_specs.append(pl.BlockSpec(memory_space=pl.ANY))
        operands.append(so_far)
        aliases = {3: 1}
    return pl.pallas_call(
        down_kernel,
        grid=(count,),
        in_specs=in_specs,
        out_specs=[
            pl.BlockSpec(
                (spread, 1, experts, own, width),
                lambda g: (0, g // per_tp, 0, 0, g % per_tp),
            ),
            pl.BlockSpec((1, width, block), lambda g: (0, g * pieces + piece, 0)),
        ],
        out_shape=[
            jax.ShapeDtypeStruct(
                (spread, tp_count, experts, own, per_tp * width), jnp.bfloat16
            ),
            jax.ShapeDtypeStruct((1, count * width * pieces, block), jnp.bfloat16),
        ],
        input_output_aliases=aliases,
        compiler_params=pltpu.CompilerParams(vmem_limit_bytes=VMEM_LIMIT),
        cost_estimate=pl.CostEstimate(
            flops=2 * tokens * count * width * block,
            bytes_accessed=count * width * block * 4 + tokens * count * width * 4,
            transcendentals=0,
        ),
    )(*operands)


def swap(pieces):
    return lax.all_to_all(pieces, "fs", split_axis=0, concat_axis=0, tiled=True)


def per_device(tokens, routes, route_logits, norm_gain, gate_weight, up_weight, down_weight):
    experts, width, _ = gate_weight.shape
    fs_count, tp_count = lax.axis_size("fs"), lax.axis_size("tp")
    spread = fs_count // experts
    own, model = tokens.shape
    part_width = model // tp_count
    pieces = 2 if width % 256 == 0 else 1
    rows, weights, gate_local, up_local, down_local, rest = exchange(
        tokens, routes, route_logits, norm_gain[:, None],
        gate_weight, up_weight, down_weight, fs_count, tp_count, pieces,
    )
    rows = rows.reshape(tp_count, fs_count * own, part_width)
    mine = lax.axis_index("fs") // spread
    weight = lax.dynamic_slice_in_dim(weights.reshape(fs_count * own, -1), mine, 1, 1)
    locals_ = [down_local]
    if pieces > 1:
        locals_.append(swap(rest))
    gate_act, gate_out = project(rows, gate_local)
    hidden, up_out = project(rows, up_local, gate_act)
    down_out, sums = None, []
    for p in range(pieces):
        part, down_out = project_back(
            hidden, weight, locals_[p], down_out, p, pieces, experts, spread, tp_count
        )
        summed = reduce(part, fs_count, tp_count)
        sums.append(summed.reshape(own, part_width // width, 1, width // pieces))
    mixed = jnp.concatenate(sums, axis=2).reshape(own, part_width)
    return (mixed, gate_out, up_out, down_out)


def solution(mesh):
    in_specs = (
        P("fs", None),
        P("fs", None),
        P("fs", None),
        P("fs"),
        P(None, "fs", "tp"),
        P(None, "fs", "tp"),
        P(None, "fs", "tp"),
    )
    out_specs = (P("fs", "tp"), P("tp", None, "fs"), P("tp", None, "fs"), P("tp", None, "fs"))
    return jax.shard_map(
        per_device, mesh=mesh, in_specs=in_specs, out_specs=out_specs, check_vma=False
    )
```

```python
import functools

import jax
import jax.numpy as jnp
from jax import lax
from jax.experimental import pallas as pl
from jax.experimental.pallas import tpu as pltpu
from jax.sharding import PartitionSpec as P

VMEM_LIMIT = 40 * 1024 * 1024


MESH = pl.DeviceIdType.MESH


def exchange_kernel(
    fs_count, tp_count, experts,
    tok_ref, routes_ref, logits_ref, gain_ref, gate_hbm, up_hbm, down_hbm,
    rows_out, weights_out, gate_out, up_out, down_out, rest_out,
    xcol, wown, stage, gate_send, up_send, down_send, rest_send,
    load_sem, send_sem, recv_sem, keep_sem, x_send, x_recv, w_send, w_recv, t_send, t_recv,
    own_sem, rest_sem,
):
    me, my_tp = lax.axis_index("fs"), lax.axis_index("tp")
    spread = fs_count // experts
    own = tok_ref.shape[0]
    width, block = stage.shape[1], stage.shape[2]
    part = xcol.shape[2]
    rows = down_send.shape[1]
    barrier = pltpu.get_barrier_semaphore()
    for s in range(1, fs_count):
        pl.semaphore_signal(
            barrier, inc=1, device_id={"fs": lax.rem(me + s, fs_count)}, device_id_type=MESH
        )
    for s in range(1, tp_count):
        pl.semaphore_signal(
            barrier, inc=1, device_id={"tp": lax.rem(my_tp + s, tp_count)}, device_id_type=MESH
        )

    def target(step):
        ahead = 1 - 2 * (2 * me // fs_count)
        return lax.rem(me + fs_count + ahead * (1 + step), fs_count)

    def load(hbm, step, slot):
        dst = target(step)
        column = pl.multiple_of(lax.rem(dst, spread) * block, block)
        return pltpu.make_async_copy(
            hbm.at[dst // spread, :, pl.ds(column, block)], stage.at[slot], load_sem.at[slot]
        )

    load(gate_hbm, 0, 0).start()

    tok = tok_ref[...].astype(jnp.float32)
    scale = lax.rsqrt(jnp.mean(tok * tok, axis=1, keepdims=True) + 1e-05)
    cols = tok_ref[:, pl.ds(pl.multiple_of(my_tp * part, part), part)].astype(jnp.float32)
    xcol[me] = (cols * scale).astype(jnp.bfloat16)
    first, second = logits_ref[0:1, :], logits_ref[1:2, :]
    ids = lax.broadcasted_iota(jnp.int32, wown.shape, 0)
    wown[...] = jnp.where(
        routes_ref[0:1, :] == ids, 1.0 / (1.0 + jnp.exp(second - first)), 0.0
    ) + jnp.where(routes_ref[1:2, :] == ids, 1.0 / (1.0 + jnp.exp(first - second)), 0.0)
    pl.semaphore_wait(barrier, fs_count + tp_count - 2)

    def x_copy(dst, sem):
        return pltpu.make_async_remote_copy(
            src_ref=xcol.at[me], dst_ref=xcol.at[me], send_sem=x_send.at[dst],
            recv_sem=x_recv.at[sem], device_id={"fs": dst}, device_id_type=MESH,
        )

    def w_copy(dst, sem):
        return pltpu.make_async_remote_copy(
            src_ref=wown, dst_ref=weights_out.at[me], send_sem=w_send.at[dst],
            recv_sem=w_recv.at[sem], device_id={"fs": dst}, device_id_type=MESH,
        )

    w_keep = pltpu.make_async_copy(wown, weights_out.at[me], own_sem.at[0])
    w_keep.start()
    for s in range(1, fs_count):
        dst = lax.rem(me + s, fs_count)
        x_copy(dst, me).start()
        w_copy(dst, me).start()

    weights_in = (
        (gate_hbm, gate_send, gate_out, True),
        (up_hbm, up_send, up_out, True),
        (down_hbm, down_send, down_out, False),
    )

    def w_send_copy(m, dst):
        _, held, out, _ = weights_in[m]
        return pltpu.make_async_remote_copy(
            src_ref=held.at[dst], dst_ref=out.at[me], send_sem=send_sem.at[m, dst],
            recv_sem=recv_sem.at[m, me], device_id={"fs": dst}, device_id_type=MESH,
        )

    def keep_copy(m):
        _, held, out, _ = weights_in[m]
        return pltpu.make_async_copy(held.at[me], out.at[me], keep_sem.at[m])

    t_copies = []
    for m in range(3):
        hbm, held, out, folded = weights_in[m]

        def body(step, carry, m=m, hbm=hbm, held=held, folded=folded):
            slot = lax.rem(m * fs_count + step, 2)
            dst = target(step)

            @pl.when(step + 1 < fs_count)
            def _():
                load(hbm, step + 1, 1 - slot).start()

            if m < 2:

                @pl.when(step + 1 == fs_count)
                def _():
                    load(weights_in[m + 1][0], 0, 1 - slot).start()

            load(hbm, step, slot).wait()
            if folded:
                held[dst] = (stage[slot] * gain_ref[...]).astype(jnp.bfloat16)
            else:
                held[dst] = stage[slot, :rows].astype(jnp.bfloat16)
                if rows < width:
                    rest_send[dst] = stage[slot, rows:].astype(jnp.bfloat16)

            @pl.when(dst == me)
            def _():
                keep_copy(m).start()

            @pl.when(dst != me)
            def _():
                w_send_copy(m, dst).start()

            return carry

        lax.fori_loop(0, fs_count, body, 0)
        if m == 0:
            for s in range(1, fs_count):
                src = lax.rem(me + s, fs_count)
                pltpu.make_async_copy(xcol.at[src], xcol.at[src], x_recv.at[src]).wait()
            for s in range(1, tp_count):
                copy = pltpu.make_async_remote_copy(
                    src_ref=xcol, dst_ref=rows_out.at[my_tp], send_sem=t_send.at[s],
                    recv_sem=t_recv.at[s], device_id={"tp": lax.rem(my_tp + s, tp_count)},
                    device_id_type=MESH,
                )
                copy.start()
                t_copies.append(copy)
            x_keep = pltpu.make_async_copy(xcol, rows_out.at[my_tp], own_sem.at[1])
            x_keep.start()
    if rows < width:
        rest_copy = pltpu.make_async_copy(rest_send, rest_out, rest_sem)
        rest_copy.start()
        rest_copy.wait()
    w_keep.wait()
    x_keep.wait()
    for s in range(1, tp_count):
        src = lax.rem(my_tp + tp_count - s, tp_count)
        t_copies[s - 1].wait_send()
        pltpu.make_async_copy(xcol, rows_out.at[src], t_recv.at[s]).wait()
    for s in range(1, fs_count):
        other = lax.rem(me + s, fs_count)
        x_copy(other, me).wait_send()
        w_copy(other, me).wait_send()
        pltpu.make_async_copy(wown, weights_out.at[other], w_recv.at[other]).wait()
    for m in range(3):
        _, held, out, _ = weights_in[m]
        keep_copy(m).wait()

        def finish(s, carry, m=m, held=held, out=out):
            other = lax.rem(me + s, fs_count)
            w_send_copy(m, other).wait_send()
            pltpu.make_async_copy(held.at[other], out.at[other], recv_sem.at[m, other]).wait()
            return carry

        lax.fori_loop(1, fs_count, finish, 0)


def exchange(tokens, routes, logits, gain, gate, up, down, fs_count, tp_count, rows):
    experts, width, columns = gate.shape
    block = columns // (fs_count // experts)
    left = width - rows if rows < width else width
    lines = -(-experts // 8) * 8
    own, model = tokens.shape
    part = model // tp_count
    bf16, dma = jnp.bfloat16, pltpu.SemaphoreType.DMA
    vmem = pl.BlockSpec(memory_space=pltpu.VMEM)
    anywhere = pl.BlockSpec(memory_space=pl.ANY)
    return pl.pallas_call(
        functools.partial(exchange_kernel, fs_count, tp_count, experts),
        in_specs=[vmem] * 4 + [anywhere] * 3,
        out_specs=[anywhere] * 6,
        out_shape=[
            jax.ShapeDtypeStruct((tp_count, fs_count, own, part), bf16),
            jax.ShapeDtypeStruct((fs_count, lines, own), jnp.float32),
            jax.ShapeDtypeStruct((fs_count, width, block), bf16),
            jax.ShapeDtypeStruct((fs_count, width, block), bf16),
            jax.ShapeDtypeStruct((fs_count, rows, block), bf16),
            jax.ShapeDtypeStruct((fs_count, left, block), bf16),
        ],
        scratch_shapes=[
            pltpu.VMEM((fs_count, own, part), bf16),
            pltpu.VMEM((lines, own), jnp.float32),
            pltpu.VMEM((2, width, block), jnp.float32),
            pltpu.VMEM((fs_count, width, block), bf16),
            pltpu.VMEM((fs_count, width, block), bf16),
            pltpu.VMEM((fs_count, rows, block), bf16),
            pltpu.VMEM((fs_count, left, block), bf16),
            dma((2,)), dma((3, fs_count)), dma((3, fs_count)), dma((3,)),
            dma((fs_count,)), dma((fs_count,)), dma((fs_count,)), dma((fs_count,)),
            dma((tp_count,)), dma((tp_count,)), dma((2,)), dma,
        ],
        compiler_params=pltpu.CompilerParams(
            collective_id=0, has_side_effects=True, vmem_limit_bytes=56 * 1024 * 1024
        ),
    )(tokens, routes, logits, gain, gate, up, down)


def reduce_kernel(
    fs_count, tp_count, experts, part_ref, out_ref, first, total, second,
    send1, recv1, send2, recv2, keep_sem,
):
    me, my_tp = lax.axis_index("fs"), lax.axis_index("tp")
    spread = fs_count // experts
    mine, half = me // spread, lax.rem(me, spread)
    group = spread * tp_count
    index = half * tp_count + my_tp
    barrier = pltpu.get_barrier_semaphore()

    def mate(s):
        other = lax.rem(index + s, group)
        return other, other // tp_count, lax.rem(other, tp_count)

    def partner(s):
        return lax.rem(mine + s, experts)

    for s in range(1, group):
        _, h, t = mate(s)
        pl.semaphore_signal(
            barrier, inc=1, device_id={"fs": mine * spread + h, "tp": t}, device_id_type=MESH
        )
    for s in range(1, experts):
        pl.semaphore_signal(
            barrier, inc=1, device_id={"fs": partner(s) * spread + half}, device_id_type=MESH
        )
    pl.semaphore_wait(barrier, group + experts - 2)

    def copy1(s):
        _, h, t = mate(s)
        return pltpu.make_async_remote_copy(
            src_ref=part_ref.at[h, t], dst_ref=first.at[s], send_sem=send1.at[s],
            recv_sem=recv1.at[s], device_id={"fs": mine * spread + h, "tp": t},
            device_id_type=MESH,
        )

    for s in range(1, group):
        copy1(s).start()
    keep = pltpu.make_async_copy(part_ref.at[half, my_tp], first.at[0], keep_sem)
    keep.start()
    keep.wait()
    acc = first[0].astype(jnp.float32)
    for s in range(1, group):
        copy1(s).wait_recv()
        acc = acc + first[s].astype(jnp.float32)
    total[...] = acc.astype(jnp.bfloat16)

    def copy2(s):
        return pltpu.make_async_remote_copy(
            src_ref=total.at[partner(s)], dst_ref=second.at[s], send_sem=send2.at[s],
            recv_sem=recv2.at[s], device_id={"fs": partner(s) * spread + half},
            device_id_type=MESH,
        )

    for s in range(1, experts):
        copy2(s).start()
    result = total[mine].astype(jnp.float32)
    for s in range(1, experts):
        copy2(s).wait_recv()
        result = result + second[s].astype(jnp.float32)
    out_ref[...] = result.astype(jnp.bfloat16)
    for s in range(1, group):
        copy1(s).wait_send()
    for s in range(1, experts):
        copy2(s).wait_send()


def reduce(part, fs_count, tp_count, number):
    spread, _, experts, own, columns = part.shape
    group = spread * tp_count
    bf16, dma = jnp.bfloat16, pltpu.SemaphoreType.DMA
    return pl.pallas_call(
        functools.partial(reduce_kernel, fs_count, tp_count, experts),
        in_specs=[pl.BlockSpec(memory_space=pltpu.VMEM)],
        out_specs=pl.BlockSpec(memory_space=pltpu.VMEM),
        out_shape=jax.ShapeDtypeStruct((own, columns), bf16),
        scratch_shapes=[
            pltpu.VMEM((group, experts, own, columns), bf16),
            pltpu.VMEM((experts, own, columns), bf16),
            pltpu.VMEM((experts, own, columns), bf16),
            dma((group,)), dma((group,)), dma((experts,)), dma((experts,)), dma,
        ],
        compiler_params=pltpu.CompilerParams(
            collective_id=number, has_side_effects=True, vmem_limit_bytes=48 * 1024 * 1024
        ),
    )(part)


def gate_kernel(x_ref, w_ref, act_ref, copy_ref):
    copy_ref[...] = w_ref[...]
    part = jnp.dot(x_ref[0], w_ref[0], preferred_element_type=jnp.float32)

    @pl.when(pl.program_id(0) == 0)
    def _():
        act_ref[...] = part

    @pl.when(pl.program_id(0) > 0)
    def _():
        act_ref[...] += part


def up_kernel(x_ref, w_ref, gate_ref, hidden_ref, copy_ref, acc_ref):
    copy_ref[...] = w_ref[...]
    part = jnp.dot(x_ref[0], w_ref[0], preferred_element_type=jnp.float32)

    @pl.when(pl.program_id(0) == 0)
    def _():
        acc_ref[...] = part

    @pl.when(pl.program_id(0) > 0)
    def _():
        acc_ref[...] += part

    @pl.when(pl.program_id(0) == pl.num_programs(0) - 1)
    def _():
        gate = gate_ref[...]
        hidden_ref[...] = (gate / (1.0 + jnp.exp(-gate)) * acc_ref[...]).astype(jnp.bfloat16)


def project(rows, local, gate_act=None):
    count, width, block = local.shape
    tokens = rows.shape[1]
    per_tp = count // rows.shape[0]
    in_specs = [
        pl.BlockSpec((1, tokens, width), lambda g: (g // per_tp, 0, g % per_tp)),
        pl.BlockSpec((1, width, block), lambda g: (g, 0, 0)),
    ]
    operands = [rows, local]
    scratch = []
    kernel, act_type = gate_kernel, jnp.float32
    if gate_act is not None:
        in_specs.append(pl.BlockSpec((tokens, block), lambda g: (0, 0)))
        operands.append(gate_act)
        scratch = [pltpu.VMEM((tokens, block), jnp.float32)]
        kernel, act_type = up_kernel, jnp.bfloat16
    return pl.pallas_call(
        kernel,
        grid=(count,),
        in_specs=in_specs,
        out_specs=[
            pl.BlockSpec((tokens, block), lambda g: (0, 0)),
            pl.BlockSpec((1, width, block), lambda g: (0, g, 0)),
        ],
        out_shape=[
            jax.ShapeDtypeStruct((tokens, block), act_type),
            jax.ShapeDtypeStruct((1, count * width, block), jnp.bfloat16),
        ],
        scratch_shapes=scratch,
        compiler_params=pltpu.CompilerParams(vmem_limit_bytes=VMEM_LIMIT),
        cost_estimate=pl.CostEstimate(
            flops=2 * tokens * count * width * block,
            bytes_accessed=count * width * block * 4,
            transcendentals=0,
        ),
    )(*operands)


def down_kernel(hidden_ref, weight_ref, w_ref, *rest):
    part_ref, copy_ref = rest[-2:]
    copy_ref[:, : w_ref.shape[1]] = w_ref[...]
    part = lax.dot_general(
        hidden_ref[...], w_ref[0], (((1,), (1,)), ((), ())), preferred_element_type=jnp.float32
    )
    part = part * weight_ref[...]
    spread, _, experts, own, width = part_ref.shape
    blocks = part.reshape(experts, spread, own, width).astype(part_ref.dtype)
    for h in range(spread):
        part_ref[h, 0] = blocks[:, h]


def project_back(hidden, weight, local, so_far, full, experts, spread, tp_count):
    count, width, block = local.shape
    tokens = hidden.shape[0]
    per_tp = count // tp_count
    own = tokens // count
    in_specs = [
        pl.BlockSpec((tokens, block), lambda g: (0, 0)),
        pl.BlockSpec((tokens, 1), lambda g: (0, 0)),
        pl.BlockSpec((1, width, block), lambda g: (g, 0, 0)),
    ]
    operands = [hidden, weight, local]
    aliases = {}
    target_spec = pl.BlockSpec((1, full, block), lambda g: (0, g, 0))
    if so_far is not None:
        in_specs.append(pl.BlockSpec(memory_space=pl.ANY))
        operands.append(so_far)
        aliases = {3: 1}
        per_full = full // width
        target_spec = pl.BlockSpec(
            (1, width, block), lambda g: (0, g * per_full + per_full - 1, 0)
        )
    return pl.pallas_call(
        down_kernel,
        grid=(count,),
        in_specs=in_specs,
        out_specs=[
            pl.BlockSpec(
                (spread, 1, experts, own, width),
                lambda g: (0, g // per_tp, 0, 0, g % per_tp),
            ),
            target_spec,
        ],
        out_shape=[
            jax.ShapeDtypeStruct(
                (spread, tp_count, experts, own, per_tp * width), jnp.bfloat16
            ),
            jax.ShapeDtypeStruct((1, count * full, block), jnp.bfloat16),
        ],
        input_output_aliases=aliases,
        compiler_params=pltpu.CompilerParams(vmem_limit_bytes=VMEM_LIMIT),
        cost_estimate=pl.CostEstimate(
            flops=2 * tokens * count * width * block,
            bytes_accessed=count * width * block * 4 + tokens * count * width * 4,
            transcendentals=0,
        ),
    )(*operands)


def swap(pieces):
    return lax.all_to_all(pieces, "fs", split_axis=0, concat_axis=0, tiled=True)


def per_device(tokens, routes, route_logits, norm_gain, gate_weight, up_weight, down_weight):
    experts, width, _ = gate_weight.shape
    fs_count, tp_count = lax.axis_size("fs"), lax.axis_size("tp")
    spread = fs_count // experts
    own, model = tokens.shape
    part_width = model // tp_count
    sent_rows = width - width // 4 if width % 512 == 0 else width
    rows, weights, gate_local, up_local, down_local, rest = exchange(
        tokens, routes.T, route_logits.T, norm_gain[:, None],
        gate_weight, up_weight, down_weight, fs_count, tp_count, sent_rows,
    )
    rows = rows.reshape(tp_count, fs_count * own, part_width)
    mine = lax.axis_index("fs") // spread
    weight = lax.dynamic_slice_in_dim(weights, mine, 1, 1).reshape(fs_count * own, 1)
    locals_ = [down_local]
    if sent_rows < width:
        locals_.append(swap(rest))
    gate_act, gate_out = project(rows, gate_local)
    hidden, up_out = project(rows, up_local, gate_act)
    down_out, sums = None, []
    for number, local in enumerate(locals_, 1):
        part, down_out = project_back(
            hidden, weight, local, down_out, width, experts, spread, tp_count
        )
        summed = reduce(part, fs_count, tp_count, number)
        sums.append(summed.reshape(own, part_width // width, local.shape[1]))
    mixed = jnp.concatenate(sums, axis=2).reshape(own, part_width)
    return (mixed, gate_out, up_out, down_out)


def solution(mesh):
    in_specs = (
        P("fs", None),
        P("fs", None),
        P("fs", None),
        P("fs"),
        P(None, "fs", "tp"),
        P(None, "fs", "tp"),
        P(None, "fs", "tp"),
    )
    out_specs = (P("fs", "tp"), P("tp", None, "fs"), P("tp", None, "fs"), P("tp", None, "fs"))
    return jax.shard_map(
        per_device, mesh=mesh, in_specs=in_specs, out_specs=out_specs, check_vma=False
    )
```
